32 devices in a mesh: sp: 8 (over z, x), tp: 4 (over y, core).
Axes of the slice: x: 2, y: 2, z: 4, core: 2. Of those that a mesh axis runs over, the one named last changes fastest.
Arguments:
- tokens: bfloat16 [1024, 2048], P('sp'), may hold values from -6 to 6
- pre_gain: float32 [2048], replicated, may hold values from 0.1 to 1.9
- outer_gate: bfloat16 [2048, 1024], P('sp', 'tp'), may hold values from -0.125 to 0.125
- inner_gate: bfloat16 [2048, 1024], P('sp', 'tp'), may hold values from -0.125 to 0.125
- conv_input: bfloat16 [2048, 1024], P('sp', 'tp'), may hold values from -0.125 to 0.125
- conv_taps: float32 [3, 1024], P(None, 'tp'), may hold values from -3.5 to 3.5
- query_down: bfloat16 [2048, 768], P(None, 'tp'), may hold values from -0.088388348 to 0.088388348
- latent_down: bfloat16 [2048, 512], P(None, 'tp'), may hold values from -0.088388348 to 0.088388348
- rotary_down: bfloat16 [2048, 32], replicated, may hold values from -0.125 to 0.125
- query_gain: float32 [768], replicated, may hold values from 1 to 3
- latent_gain: float32 [512], replicated, may hold values from 1 to 3
- query_up: bfloat16 [768, 512], P(None, 'tp'), may hold values from -0.14433757 to 0.14433757
- query_rotary: bfloat16 [768, 256], P(None, 'tp'), may hold values from -0.21875 to 0.21875
- key_up: bfloat16 [512, 512], P(None, 'tp'), may hold values from -4.33012702 to 4.33012702
- value_up: bfloat16 [512, 512], P(None, 'tp'), may hold values from -0.25 to 0.25
- conv_output: bfloat16 [1024, 2048], P('tp'), may hold values from -0.15625 to 0.15625
- heads_output: bfloat16 [512, 2048], P('tp'), may hold values from -0.15625 to 0.15625
- post_gain: float32 [2048], replicated, may hold values from 0.1 to 1.9
Outputs:
- mixed: bfloat16 [1024, 2048], P(('sp', 'tp'))
- row_logsum: float32 [8, 1024], P('tp', 'sp')
The draws below stay inside these ranges and needn't reach their ends.
All inputs are finite; a program needn't handle non-finite values.
Results may differ from the reference program's by a relative error of at most 0.013.
Values may be sent and summed in bfloat16 or wider, within the bound.
A program may use at most 64 MiB of HBM per device.

```python
import math
import jax
import jax.numpy as jnp
from jax import lax

D = 2048
D_CONV = 1024
HEADS = 8
NOPE = 64
ROPE = 32
VDIM = 64
QLAT = 768
KVLAT = 512
TAPS = 3
TOKENS = 1024


def clipped(key, shape, fan_in):
    return jnp.clip(jax.random.normal(key, shape, jnp.float32), -3.95, 3.95) * fan_in ** (-0.5)


def shared_down(key):
    return clipped(jax.random.fold_in(key, 101), (D, QLAT), D)


def shared_up(key):
    return clipped(jax.random.fold_in(key, 103), (QLAT, HEADS * NOPE), QLAT)


def draw_query_down(key, part):
    return shared_down(key).astype(jnp.bfloat16)


def draw_latent_down(key, part):
    result = clipped(jax.random.fold_in(key, 102), (D, KVLAT), D)
    return result.astype(jnp.bfloat16)


def draw_query_up(key, part):
    return shared_up(key).astype(jnp.bfloat16)


def draw_key_up(key, part):
    result = clipped(jax.random.fold_in(key, 105), (KVLAT, HEADS * NOPE), KVLAT)
    return result.astype(jnp.bfloat16)


def block_levels(stream_key, shape, split, low, high):
    level = 1.0
    for dim, blocks in split:
        steps = jax.random.uniform(jax.random.fold_in(jax.random.fold_in(stream_key, 6), dim), (blocks,), jnp.float32, low / len(split), high / len(split))
        level = level * jnp.repeat(jnp.exp(steps), shape[dim] // blocks).reshape((-1,) + (1,) * (len(shape) - 1 - dim))
    return level


def gaussian(key, extent, spread, reach, shards=(), held_as=jnp.bfloat16):
    array = spread * jax.random.normal(key, extent, jnp.float32)
    if shards:
        array = array * block_levels(key, extent, shards, -0.22, 0.18)
    return jnp.clip(array, -reach, reach).astype(held_as)


def setup_inputs(seed: int = 0) -> dict:
    arg_keys = jax.random.split(jax.random.key(seed), 19)
    return {
        "tokens": gaussian(arg_keys[0], (TOKENS, D), 1.0, 6.0, ((0, 8),)),
        "pre_gain": jnp.clip(1.0 + 0.18 * jax.random.normal(arg_keys[1], (D,), jnp.float32), 0.1, 1.9),
        "outer_gate": gaussian(arg_keys[2], (D, D_CONV), D ** -0.5, 0.125, ((0, 8), (1, 4))),
        "inner_gate": gaussian(arg_keys[3], (D, D_CONV), D ** -0.5, 0.125, ((0, 8), (1, 4))),
        "conv_input": gaussian(arg_keys[4], (D, D_CONV), D ** -0.5, 0.125, ((0, 8), (1, 4))),
        "conv_taps": gaussian(arg_keys[5], (TAPS, D_CONV), TAPS ** -0.5, 3.5, ((1, 4),), jnp.float32),
        "query_down": draw_query_down(jax.random.fold_in(arg_keys[18], 71), 0),
        "latent_down": draw_latent_down(jax.random.fold_in(arg_keys[18], 71), 0),
        "rotary_down": gaussian(arg_keys[8], (D, ROPE), D ** -0.5, 0.125),
        "query_gain": jnp.clip(jnp.exp(jax.random.uniform(arg_keys[9], (QLAT,), jnp.float32, math.log(1.0), math.log(3.0))), 1.0, 3.0),
        "latent_gain": jnp.clip(jnp.exp(jax.random.uniform(arg_keys[10], (KVLAT,), jnp.float32, math.log(1.0), math.log(3.0))), 1.0, 3.0),
        "query_up": draw_query_up(jax.random.fold_in(arg_keys[18], 71), 0),
        "query_rotary": gaussian(arg_keys[12], (QLAT, HEADS * ROPE), QLAT ** -0.5, 0.21875, ((1, 4),)),
        "key_up": draw_key_up(jax.random.fold_in(arg_keys[18], 71), 0),
        "value_up": gaussian(arg_keys[14], (KVLAT, HEADS * VDIM), KVLAT ** -0.5, 0.25, ((1, 4),)),
        "conv_output": gaussian(arg_keys[15], (D_CONV, D), (D_CONV + HEADS * VDIM) ** -0.5, 0.15625, ((0, 4),)),
        "heads_output": gaussian(arg_keys[16], (HEADS * VDIM, D), (D_CONV + HEADS * VDIM) ** -0.5, 0.15625, ((0, 4),)),
        "post_gain": jnp.clip(1.0 + 0.18 * jax.random.normal(arg_keys[17], (D,), jnp.float32), 0.1, 1.9),
    }


eps = 1e-06
rope_theta = 500000.0

def rms_scale(values, scale_row):
    widened = values.astype(jnp.float32)
    return widened * lax.rsqrt(lax.optimization_barrier(jnp.mean(widened * widened, axis=-1, keepdims=True)) + eps) * scale_row

def rotate(values, positions):
    half_width = values.shape[-1] // 2
    frequency = rope_theta ** (-jnp.arange(half_width, dtype=jnp.float32) / half_width)
    angles = positions.astype(jnp.float32)[:, None] * frequency
    cosine = jnp.cos(angles)[:, None, :]
    sine_part = jnp.sin(angles)[:, None, :]
    leading = values[..., :half_width]
    trailing = values[..., half_width:]
    return jnp.concatenate([leading * cosine - trailing * sine_part, trailing * cosine + leading * sine_part], axis=-1)

def reference(tokens, pre_gain, outer_gate, inner_gate, conv_input, conv_taps, query_down, latent_down, rotary_down, query_gain, latent_gain, query_up, query_rotary, key_up, value_up, conv_output, heads_output, post_gain):
    normed = rms_scale(tokens, pre_gain).astype(jnp.bfloat16)
    positions = jnp.arange(TOKENS, dtype=jnp.int32)
    outer_part = jnp.dot(normed, outer_gate, preferred_element_type=jnp.float32)
    inner_part = jnp.dot(normed, inner_gate, preferred_element_type=jnp.float32)
    signal = jnp.dot(normed, conv_input, preferred_element_type=jnp.float32)
    product = (inner_part * signal).astype(jnp.bfloat16)
    extended = jnp.concatenate([jnp.zeros((TAPS - 1, D_CONV), jnp.float32), product.astype(jnp.float32)], axis=0)
    convolved = extended[0:TOKENS] * conv_taps[0]
    for offset in range(1, TAPS):
        convolved = convolved + extended[offset:offset + TOKENS] * conv_taps[offset]
    conv_mixed = (outer_part * convolved).astype(jnp.bfloat16)
    query_latent = jnp.dot(normed, query_down, preferred_element_type=jnp.float32).astype(jnp.bfloat16)
    key_latent = jnp.dot(normed, latent_down, preferred_element_type=jnp.float32).astype(jnp.bfloat16)
    query_normed = rms_scale(query_latent, query_gain).astype(jnp.bfloat16)
    latent_normed = rms_scale(key_latent, latent_gain).astype(jnp.bfloat16)
    rotary_raw = jnp.dot(normed, rotary_down, preferred_element_type=jnp.float32)
    key_rotary = rotate(rotary_raw[:, None, :], positions)[:, 0, :].astype(jnp.bfloat16)
    query_nope = jnp.dot(query_normed, query_up, preferred_element_type=jnp.float32).astype(jnp.bfloat16)
    query_nope = query_nope.reshape(TOKENS, HEADS, NOPE)
    turned_raw = jnp.dot(query_normed, query_rotary, preferred_element_type=jnp.float32)
    query_turned = rotate(turned_raw.reshape(TOKENS, HEADS, ROPE), positions).astype(jnp.bfloat16)
    key_nope = jnp.dot(latent_normed, key_up, preferred_element_type=jnp.float32).astype(jnp.bfloat16)
    key_nope = key_nope.reshape(TOKENS, HEADS, NOPE).astype(jnp.float32)
    value_rows = jnp.dot(latent_normed, value_up, preferred_element_type=jnp.float32).astype(jnp.bfloat16)
    value_rows = value_rows.reshape(TOKENS, HEADS, VDIM).astype(jnp.float32)
    key_wide = key_rotary.astype(jnp.float32)
    score_scale = (NOPE + ROPE) ** (-0.5)
    block_rows = 512 if TOKENS % 512 == 0 else TOKENS

    def one_block(block_index):
        first_row = block_index * block_rows
        query_block = lax.dynamic_slice_in_dim(query_nope, first_row, block_rows, 0).astype(jnp.float32)
        turned_block = lax.dynamic_slice_in_dim(query_turned, first_row, block_rows, 0).astype(jnp.float32)
        scores = jnp.einsum('qhd,khd->hqk', query_block, key_nope)
        scores = scores + jnp.einsum('qhd,kd->hqk', turned_block, key_wide)
        scores = scores * score_scale
        query_position = first_row + jnp.arange(block_rows, dtype=jnp.int32)
        causal = positions[None, :] <= query_position[:, None]
        scores = jnp.where(causal[None], scores, -1e+30)
        row_best = lax.optimization_barrier(jnp.max(scores, axis=-1))
        weights = jnp.where(causal[None], jnp.exp(scores - row_best[..., None]), 0.0)
        weight_sum = lax.optimization_barrier(jnp.sum(weights, axis=-1))
        rounded = lax.optimization_barrier(weights.astype(jnp.bfloat16))
        weighted = jnp.einsum('hqk,khd->hqd', rounded.astype(jnp.float32), value_rows)
        mixed_block = (weighted / weight_sum[..., None]).astype(jnp.bfloat16)
        return (mixed_block, row_best + jnp.log(weight_sum))
    blocks_out, logsums = lax.map(one_block, jnp.arange(TOKENS // block_rows, dtype=jnp.int32))
    heads_mixed = blocks_out.transpose(0, 2, 1, 3).reshape(TOKENS, HEADS * VDIM)
    row_logsum = logsums.transpose(1, 0, 2).reshape(HEADS, TOKENS)
    projected = jnp.dot(conv_mixed, conv_output, preferred_element_type=jnp.float32)
    projected = projected + jnp.dot(heads_mixed, heads_output, preferred_element_type=jnp.float32)
    mixed = rms_scale(projected, post_gain).astype(jnp.bfloat16)
    return (mixed, row_logsum)
```

```python
import functools

import jax
import jax.numpy as jnp
import numpy as np
from jax import lax
from jax.experimental import pallas as pl
from jax.experimental.pallas import tpu as pltpu
from jax.sharding import PartitionSpec as P

NOPE = 64
ROPE = 32
VDIM = 64
TAPS = 3
HALO = 16

eps = 1e-06
rope_theta = 500000.0
F32 = jnp.float32
BF16 = jnp.bfloat16
MESH = pl.DeviceIdType.MESH


def dot(a, b):
    return jnp.dot(a, b, preferred_element_type=F32)


def dot_nt(a, b):
    return lax.dot_general(a, b, (((1,), (1,)), ((), ())), preferred_element_type=F32)


def normalized(values, gain):
    wide = values.astype(F32)
    return wide * lax.rsqrt(jnp.mean(wide * wide, axis=-1, keepdims=True) + eps) * gain


def swapped(values):
    half = ROPE // 2
    parts = []
    for first in range(0, values.shape[-1], ROPE):
        parts += [values[:, first + half : first + ROPE], values[:, first : first + half]]
    return jnp.concatenate(parts, axis=1)


def kernel(
    sp, tp, inner,
    tokens, pre_gain, outer_gate, inner_gate, conv_input, conv_taps, query_down, latent_down,
    rotary_down, query_gain, latent_gain, query_up, query_rotary, key_up, value_up,
    conv_output, heads_output, post_gain, table,
    mixed, row_logsum,
    wbuf, normed, halo, acc, prod, qlat, klat, kvbuf, qcat, best, total, weighted, proj,
    convm, outbuf, rsbuf, wout, wheads, tab,
    local_sem, w_recv, w_send, halo_sem, lat_send, lat_recv, kv_send, kv_recv, rs_send, rs_recv,
):
    rows = tokens.shape[0]
    depth = outer_gate.shape[0]
    heads = query_up.shape[1] // NOPE
    lines = sp // inner
    me = lax.axis_index("sp")
    mine = lax.axis_index("tp")
    zi = me // inner
    xi = me % inner
    ql = query_down.shape[1]
    kl = latent_down.shape[1]

    def sp_row(slot):
        return pl.ds(pl.multiple_of(slot * depth, depth), depth)

    locals_ = [
        pltpu.make_async_copy(ref, wbuf.at[i, sp_row(me)], local_sem.at[i])
        for i, ref in enumerate((outer_gate, inner_gate, conv_input))
    ]
    locals_ += [
        pltpu.make_async_copy(
            table.at[pl.ds(pl.multiple_of(me * rows, rows), rows)], tab, local_sem.at[3]
        ),
        pltpu.make_async_copy(heads_output, wheads, local_sem.at[4]),
        pltpu.make_async_copy(conv_output, wout, local_sem.at[5]),
    ]
    for copy in locals_:
        copy.start()

    barrier = pltpu.get_barrier_semaphore()

    def greet_sp(k, carry):
        pl.semaphore_signal(barrier, inc=1, device_id={"sp": (me + k) % sp}, device_id_type=MESH)
        return carry

    lax.fori_loop(1, sp, greet_sp, 0)
    for k in range(1, tp):
        pl.semaphore_signal(barrier, inc=1, device_id={"tp": (mine + k) % tp}, device_id_type=MESH)

    normed[pl.ds(HALO, rows), :] = normalized(tokens[...], pre_gain[...]).astype(BF16)
    pl.semaphore_wait(barrier, sp + tp - 2)

    def w_copy(i, slot, way):
        if way == 2:
            target = zi * inner + (inner - 1 - xi)
        else:
            target = me + (inner if way == 0 else -inner)
        return pltpu.make_async_remote_copy(
            src_ref=wbuf.at[i, sp_row(slot)],
            dst_ref=wbuf.at[i, sp_row(slot)],
            send_sem=w_send.at[way, i, slot],
            recv_sem=w_recv.at[i, slot],
            device_id={"sp": target},
            device_id_type=MESH,
        )

    def w_wait(i, slot):
        pltpu.make_async_copy(
            wbuf.at[i, sp_row(slot)], wbuf.at[i, sp_row(slot)], w_recv.at[i, slot]
        ).wait()

    halo_copy = pltpu.make_async_remote_copy(
        src_ref=tokens.at[pl.ds(rows - HALO, HALO)],
        dst_ref=halo,
        send_sem=halo_sem.at[0],
        recv_sem=halo_sem.at[1],
        device_id={"sp": (me + 1) % sp},
        device_id_type=MESH,
    )

    @pl.when(me < sp - 1)
    def _():
        halo_copy.start()

    for i in range(3):
        locals_[i].wait()

        @pl.when(zi < lines - 1)
        def _():
            w_copy(i, me, 0).start()

        @pl.when(zi > 0)
        def _():
            w_copy(i, me, 1).start()

        w_copy(i, me, 2).start()

    own = normed[pl.ds(HALO, rows), :]
    klat[mine] = dot(own, latent_down[...]).astype(BF16)
    qlat[mine] = dot(own, query_down[...]).astype(BF16)

    def lat_copy(which, k):
        buf = (klat, qlat)[which]
        return pltpu.make_async_remote_copy(
            src_ref=buf.at[mine],
            dst_ref=buf.at[mine],
            send_sem=lat_send.at[which, k],
            recv_sem=lat_recv.at[which, mine],
            device_id={"tp": (mine + k) % tp},
            device_id_type=MESH,
        )

    for which in range(2):
        for k in range(1, tp):
            lat_copy(which, k).start()

    rotary_raw = dot(own, rotary_down[...])

    @pl.when(me == 0)
    def _():
        normed[pl.ds(0, HALO), :] = jnp.zeros((HALO, normed.shape[1]), BF16)

    @pl.when(me > 0)
    def _():
        halo_copy.wait_recv()
        normed[pl.ds(0, HALO), :] = normalized(halo[...], pre_gain[...]).astype(BF16)

    locals_[3].wait()
    width = heads * ROPE
    cosine, sine = tab[:, :width], tab[:, width : 2 * width]
    key_rotary = (
        rotary_raw * cosine[:, :ROPE] + swapped(rotary_raw) * sine[:, :ROPE]
    ).astype(BF16)

    def lat_wait(which):
        buf = (klat, qlat)[which]
        for k in range(1, tp):
            other = (mine + k) % tp
            pltpu.make_async_copy(buf.at[other], buf.at[other], lat_recv.at[which, other]).wait()

    lat_wait(0)
    latent = jnp.concatenate([klat[t] for t in range(tp)], axis=1)
    latent_normed = normalized(latent, latent_gain[...]).astype(BF16)
    key_nope = dot(latent_normed, key_up[...]).astype(BF16)
    values = dot(latent_normed, value_up[...]).astype(BF16)
    tail = kvbuf.shape[3] - NOPE - ROPE
    blank = [jnp.zeros((rows, tail), BF16)] if tail else []
    for h in range(heads):
        kvbuf[me, h] = jnp.concatenate(
            [key_nope[:, h * NOPE : (h + 1) * NOPE], key_rotary] + blank, axis=1
        )
    kvbuf[me, heads] = values

    def kv_copy(target):
        return pltpu.make_async_remote_copy(
            src_ref=kvbuf.at[me],
            dst_ref=kvbuf.at[me],
            send_sem=kv_send.at[target],
            recv_sem=kv_recv.at[me],
            device_id={"sp": target},
            device_id_type=MESH,
        )

    def kv_start(target, carry):
        kv_copy(target).start()
        return carry

    lax.fori_loop(me + 1, sp, kv_start, 0)

    lat_wait(1)
    wide = [qlat[t].astype(F32) for t in range(tp)]
    squares = sum(jnp.sum(w * w, axis=-1, keepdims=True) for w in wide)
    scale = lax.rsqrt(squares / (ql * tp) + eps)
    query_nope = jnp.zeros((rows, heads * NOPE), F32)
    turned = jnp.zeros((rows, width), F32)
    for t in range(tp):
        piece = (wide[t] * scale * query_gain[t : t + 1, :]).astype(BF16)
        query_nope = query_nope + dot(piece, query_up[t * ql : (t + 1) * ql, :])
        turned = turned + dot(piece, query_rotary[t * ql : (t + 1) * ql, :])
    query_nope = query_nope.astype(BF16)
    turned = (turned * cosine + swapped(turned) * sine).astype(BF16)
    for h in range(heads):
        qcat[h] = jnp.concatenate(
            [
                query_nope[:, h * NOPE : (h + 1) * NOPE],
                turned[:, h * ROPE : (h + 1) * ROPE],
            ]
            + blank,
            axis=1,
        )

    aligned = depth % 128 == 0

    def gate_step(i, slot, first=False):
        columns = pl.ds(pl.multiple_of(slot * depth, depth), depth)
        value = dot(normed[:, columns], wbuf[i, sp_row(slot), :])
        if first:
            acc[i] = value
        else:
            acc[i] += value

    if aligned:
        for i in range(3):
            gate_step(i, me, True)

    def line_step(d, carry):
        for i in range(3):

            @pl.when(zi - d >= 0)
            def _():
                slot = me - d * inner
                w_wait(i, slot)

                @pl.when(zi < lines - 1)
                def _():
                    w_copy(i, slot, 0).start()

                w_copy(i, slot, 2).start()

            @pl.when(zi + d <= lines - 1)
            def _():
                slot = me + d * inner
                w_wait(i, slot)

                @pl.when(zi > 0)
                def _():
                    w_copy(i, slot, 1).start()

                w_copy(i, slot, 2).start()

        if aligned:

            @pl.when(zi - d >= 0)
            def _():
                for i in range(3):
                    gate_step(i, me - d * inner)

            @pl.when(zi + d <= lines - 1)
            def _():
                for i in range(3):
                    gate_step(i, me + d * inner)

        return carry

    lax.fori_loop(1, lines, line_step, 0)

    factor = (NOPE + ROPE) ** (-0.5)
    row_id = lax.broadcasted_iota(jnp.int32, (rows, rows), 0)
    key_id = lax.broadcasted_iota(jnp.int32, (rows, rows), 1)
    for h in range(heads):
        scores = dot_nt(qcat[h], kvbuf[me, h]) * factor
        scores = jnp.where(key_id <= row_id, scores, -1e30)
        top = jnp.max(scores, axis=-1, keepdims=True)
        weights = jnp.where(key_id <= row_id, jnp.exp(scores - top), 0.0)
        best[h] = top
        total[h] = jnp.sum(weights, axis=-1, keepdims=True)
        weighted[h] = dot(weights.astype(BF16), kvbuf[me, heads])

    def attend(k, carry):
        slot = me - k
        pltpu.make_async_copy(kvbuf.at[slot], kvbuf.at[slot], kv_recv.at[slot]).wait()
        for h in range(heads):
            scores = dot_nt(qcat[h], kvbuf[slot, h]) * factor
            old = best[h]
            top = jnp.maximum(old, jnp.max(scores, axis=-1, keepdims=True))
            weights = jnp.exp(scores - top)
            shrink = jnp.exp(old - top)
            best[h] = top
            total[h] = total[h] * shrink + jnp.sum(weights, axis=-1, keepdims=True)
            weighted[h] = weighted[h] * shrink + dot(weights.astype(BF16), kvbuf[slot, heads])
        return carry

    lax.fori_loop(1, me + 1, attend, 0)
    lane = lax.broadcasted_iota(jnp.int32, (rows, heads * VDIM), 1)
    heads_mixed = jnp.zeros((rows, heads * VDIM), F32)
    for h in range(heads):
        logsum = best[h] + jnp.log(total[h])
        row_logsum[h : h + 1, :] = jnp.transpose(jnp.broadcast_to(logsum, (rows, rows)))[0:1, :]
        heads_mixed = jnp.where(lane // VDIM == h, weighted[h] / total[h], heads_mixed)
    locals_[4].wait()
    proj[...] = dot(heads_mixed.astype(BF16), wheads[...])

    other_x = inner - 1 - xi

    def pair_slot(slot):
        for i in range(3):
            w_wait(i, slot)
            if aligned:
                gate_step(i, slot)

    pair_slot(zi * inner + other_x)

    def pair_step(d, carry):
        @pl.when(zi - d >= 0)
        def _():
            pair_slot((zi - d) * inner + other_x)

        @pl.when(zi + d <= lines - 1)
        def _():
            pair_slot((zi + d) * inner + other_x)

        return carry

    lax.fori_loop(1, lines, pair_step, 0)
    if not aligned:
        for i in range(3):
            acc[i] = dot(normed[...], wbuf[i])

    prod[...] = (acc[1] * acc[2]).astype(BF16).astype(F32)
    convolved = prod[pl.ds(HALO - TAPS + 1, rows), :] * conv_taps[0:1, :]
    for k in range(1, TAPS):
        convolved = convolved + prod[pl.ds(HALO - TAPS + 1 + k, rows), :] * conv_taps[k : k + 1, :]
    convm[...] = (acc[0, pl.ds(HALO, rows), :] * convolved).astype(BF16)

    locals_[5].wait()
    part = rows // tp

    def share(target):
        where = pl.ds(pl.multiple_of(target * part, part), part)
        return proj[where, :] + dot(convm[where, :], wout[...])

    def rs_copy(k):
        return pltpu.make_async_remote_copy(
            src_ref=outbuf.at[k],
            dst_ref=rsbuf.at[mine],
            send_sem=rs_send.at[k],
            recv_sem=rs_recv.at[mine],
            device_id={"tp": (mine + k) % tp},
            device_id_type=MESH,
        )

    order = sorted(range(1, tp), key=lambda k: abs(k - tp // 2))
    for k in order:
        outbuf[k] = share((mine + k) % tp).astype(BF16)
        rs_copy(k).start()
    result = share(mine)
    for k in range(1, tp):
        other = (mine + k) % tp
        pltpu.make_async_copy(rsbuf.at[other], rsbuf.at[other], rs_recv.at[other]).wait()
        result = result + rsbuf[other].astype(F32)
    mixed[...] = normalized(result, post_gain[...]).astype(BF16)

    for k in range(1, tp):
        rs_copy(k).wait_send()
        for which in range(2):
            lat_copy(which, k).wait_send()

    @pl.when(me < sp - 1)
    def _():
        halo_copy.wait_send()

    def kv_end(target, carry):
        kv_copy(target).wait_send()
        return carry

    lax.fori_loop(me + 1, sp, kv_end, 0)

    def w_end(z, carry):
        slot = z * inner + xi
        for i in range(3):
            w_copy(i, slot, 2).wait_send()

            @pl.when((z <= zi) & (zi < lines - 1))
            def _():
                w_copy(i, slot, 0).wait_send()

            @pl.when((z >= zi) & (zi > 0))
            def _():
                w_copy(i, slot, 1).wait_send()

        return carry

    lax.fori_loop(0, lines, w_end, 0)


def rope_table(count, heads):
    half = ROPE // 2
    frequency = np.float32(rope_theta) ** (-np.arange(half, dtype=np.float32) / np.float32(half))
    angles = np.arange(count, dtype=np.float32)[:, None] * frequency.astype(np.float32)
    cosine, sine = np.cos(angles), np.sin(angles)
    both = [np.concatenate([cosine, cosine], 1)] * heads + [np.concatenate([-sine, sine], 1)] * heads
    return np.concatenate(both, axis=1).astype(np.float32)


def solution(mesh):
    sp, tp = mesh.shape["sp"], mesh.shape["tp"]
    inner = 2

    def local(
        tokens, pre_gain, outer_gate, inner_gate, conv_input, conv_taps, query_down, latent_down,
        rotary_down, query_gain, latent_gain, query_up, query_rotary, key_up, value_up,
        conv_output, heads_output, post_gain,
    ):
        rows, model = tokens.shape
        depth, channels = outer_gate.shape
        heads = query_up.shape[1] // NOPE
        ql, kl = query_down.shape[1], latent_down.shape[1]
        slab = max(heads * VDIM, 128)
        part = rows // tp
        table = jnp.asarray(rope_table(rows * sp, heads))
        vm = pl.BlockSpec(memory_space=pltpu.VMEM)
        hbm = pl.BlockSpec(memory_space=pl.ANY)
        dma = pltpu.SemaphoreType.DMA
        return pl.pallas_call(
            functools.partial(kernel, sp, tp, inner),
            out_shape=(
                jax.ShapeDtypeStruct((part, model), BF16),
                jax.ShapeDtypeStruct((heads, rows), F32),
            ),
            in_specs=[
                vm, vm, hbm, hbm, hbm, vm, vm, vm, vm, vm, vm, vm, vm, vm, vm, hbm, hbm, vm, hbm,
            ],
            out_specs=(vm, vm),
            scratch_shapes=[
                pltpu.VMEM((3, sp * depth, channels), BF16),
                pltpu.VMEM((rows + HALO, model), BF16),
                pltpu.VMEM((HALO, model), BF16),
                pltpu.VMEM((3, rows + HALO, channels), F32),
                pltpu.VMEM((rows + HALO, channels), F32),
                pltpu.VMEM((tp, rows, ql), BF16),
                pltpu.VMEM((tp, rows, kl), BF16),
                pltpu.VMEM((sp, heads + 1, rows, slab), BF16),
                pltpu.VMEM((heads, rows, slab), BF16),
                pltpu.VMEM((heads, rows, 1), F32),
                pltpu.VMEM((heads, rows, 1), F32),
                pltpu.VMEM((heads, rows, heads * VDIM), F32),
                pltpu.VMEM((rows, model), F32),
                pltpu.VMEM((rows, channels), BF16),
                pltpu.VMEM((tp, part, model), BF16),
                pltpu.VMEM((tp, part, model), BF16),
                pltpu.VMEM(conv_output.shape, BF16),
                pltpu.VMEM(heads_output.shape, BF16),
                pltpu.VMEM((rows, 2 * heads * ROPE), F32),
                dma((6,)),
                dma((3, sp)),
                dma((3, 3, sp)),
                dma((2,)),
                dma((2, tp)),
                dma((2, tp)),
                dma((sp,)),
                dma((sp,)),
                dma((tp,)),
                dma((tp,)),
            ],
            compiler_params=pltpu.CompilerParams(collective_id=0, has_side_effects=True),
        )(
            tokens, pre_gain.reshape(1, -1), outer_gate, inner_gate, conv_input, conv_taps,
            query_down, latent_down, rotary_down, query_gain.reshape(tp, ql),
            latent_gain.reshape(1, -1), query_up, query_rotary, key_up, value_up,
            conv_output, heads_output, post_gain.reshape(1, -1), table,
        )

    in_specs = (
        P("sp", None), P(), P("sp", "tp"), P("sp", "tp"), P("sp", "tp"), P(None, "tp"),
        P(None, "tp"), P(None, "tp"), P(), P(), P(), P(None, "tp"), P(None, "tp"),
        P(None, "tp"), P(None, "tp"), P("tp", None), P("tp", None), P(),
    )
    out_specs = (P(("sp", "tp"), None), P("tp", "sp"))
    return jax.shard_map(local, mesh=mesh, in_specs=in_specs, out_specs=out_specs, check_vma=False)
```

```python
import functools

import jax
import jax.numpy as jnp
import numpy as np
from jax import lax
from jax.experimental import pallas as pl
from jax.experimental.pallas import tpu as pltpu
from jax.sharding import PartitionSpec as P

NOPE = 64
ROPE = 32
VDIM = 64
TAPS = 3
HALO = 16

eps = 1e-06
rope_theta = 500000.0
F32 = jnp.float32
BF16 = jnp.bfloat16
MESH = pl.DeviceIdType.MESH


def dot(a, b):
    return jnp.dot(a, b, preferred_element_type=F32)


def dot_nt(a, b):
    return lax.dot_general(a, b, (((1,), (1,)), ((), ())), preferred_element_type=F32)


def normalized(values, gain):
    wide = values.astype(F32)
    return wide * lax.rsqrt(jnp.mean(wide * wide, axis=-1, keepdims=True) + eps) * gain


def swapped(values):
    half = ROPE // 2
    parts = []
    for first in range(0, values.shape[-1], ROPE):
        parts += [values[:, first + half : first + ROPE], values[:, first : first + half]]
    return jnp.concatenate(parts, axis=1)


def kernel(
    sp, tp, inner,
    tokens, pre_gain, outer_gate, inner_gate, conv_input, conv_taps, query_down, latent_down,
    rotary_down, query_gain, latent_gain, query_up, query_rotary, key_up, value_up,
    conv_output, heads_output, post_gain, table, key_table,
    mixed, row_logsum,
    wbuf, normed, halo, acc, prod, qlat, latbuf, qnope, qturn, best, total, weighted, proj,
    convm, outbuf, rsbuf, wout, wheads, tab, key_tab,
    local_sem, w_recv, w_send, halo_sem, q_send, q_recv, lat_send, lat_recv, sp_send,
    rs_send, rs_recv,
):
    rows = tokens.shape[0]
    depth = outer_gate.shape[0]
    heads = query_up.shape[1] // NOPE
    lines = sp // inner
    me = lax.axis_index("sp")
    mine = lax.axis_index("tp")
    zi = me // inner
    xi = me % inner
    ql = query_down.shape[0]
    channels = outer_gate.shape[1]
    units = w_units(channels)
    kl = latent_down.shape[1]

    def sp_row(slot):
        return pl.ds(pl.multiple_of(slot * depth, depth), depth)

    locals_ = [
        pltpu.make_async_copy(ref, wbuf.at[i, sp_row(me)], local_sem.at[i])
        for i, ref in enumerate((outer_gate, inner_gate, conv_input))
    ]
    locals_ += [
        pltpu.make_async_copy(table.at[me], tab, local_sem.at[3]),
        pltpu.make_async_copy(key_table.at[me], key_tab, local_sem.at[6]),
        pltpu.make_async_copy(heads_output, wheads, local_sem.at[4]),
        pltpu.make_async_copy(conv_output, wout, local_sem.at[5]),
    ]
    for copy in locals_:
        copy.start()

    barrier = pltpu.get_barrier_semaphore()

    def greet_sp(k, carry):
        pl.semaphore_signal(barrier, inc=1, device_id={"sp": (me + k) % sp}, device_id_type=MESH)
        return carry

    lax.fori_loop(1, sp, greet_sp, 0)
    for k in range(1, tp):
        pl.semaphore_signal(barrier, inc=1, device_id={"tp": (mine + k) % tp}, device_id_type=MESH)

    normed[pl.ds(HALO, rows), :] = normalized(tokens[...], pre_gain[...]).astype(BF16)
    pl.semaphore_wait(barrier, sp + tp - 2)

    def w_part(u, slot):
        i, first, size = units[u]
        return wbuf.at[i, sp_row(slot), pl.ds(first, size)]

    def w_copy(u, slot, way):
        if way == 2:
            target = zi * inner + (inner - 1 - xi)
        else:
            target = me + (inner if way == 0 else -inner)
        return pltpu.make_async_remote_copy(
            src_ref=w_part(u, slot),
            dst_ref=w_part(u, slot),
            send_sem=w_send.at[way, u, slot],
            recv_sem=w_recv.at[u, slot],
            device_id={"sp": target},
            device_id_type=MESH,
        )

    def w_wait(u, slot):
        pltpu.make_async_copy(w_part(u, slot), w_part(u, slot), w_recv.at[u, slot]).wait()

    def up(u, slot):
        @pl.when(zi < lines - 1)
        def _():
            w_copy(u, slot, 0).start()

    def down(u, slot):
        @pl.when(zi > 0)
        def _():
            w_copy(u, slot, 1).start()

    late = len(units) - 1
    pair = zi * inner + (inner - 1 - xi)

    halo_copy = pltpu.make_async_remote_copy(
        src_ref=tokens.at[pl.ds(rows - HALO, HALO)],
        dst_ref=halo,
        send_sem=halo_sem.at[0],
        recv_sem=halo_sem.at[1],
        device_id={"sp": (me + 1) % sp},
        device_id_type=MESH,
    )

    @pl.when(me < sp - 1)
    def _():
        halo_copy.start()

    for i in range(3):
        locals_[i].wait()
    w_copy(late, me, 2).start()
    for u in range(late):
        up(u, me)
        down(u, me)
        w_copy(u, me, 2).start()
    up(late, me)
    down(late, me)

    own = normed[pl.ds(HALO, rows), :]
    latbuf[me, mine, 0:rows, 0:kl] = dot(own, latent_down[...]).astype(BF16)
    key_raw = dot_nt(rotary_down[...], own)
    half = ROPE // 2
    locals_[4].wait()
    key_swap = jnp.concatenate([key_raw[half:], key_raw[:half]], axis=0)
    key_rotary = key_raw * key_tab[0:ROPE, :] + key_swap * key_tab[ROPE : 2 * ROPE, :]
    latbuf[me, mine, rows : rows + ROPE, 0:rows] = key_rotary.astype(BF16)

    def lat_part(slot, t):
        return latbuf.at[slot, t, pl.ds(0, rows)]

    def lat_copy(slot, k):
        return pltpu.make_async_remote_copy(
            src_ref=lat_part(slot, mine),
            dst_ref=lat_part(slot, mine),
            send_sem=lat_send.at[slot, k],
            recv_sem=lat_recv.at[slot, mine],
            device_id={"tp": (mine + k) % tp},
            device_id_type=MESH,
        )

    def lat_wait(slot):
        for k in range(1, tp):
            t = (mine + k) % tp
            pltpu.make_async_copy(lat_part(slot, t), lat_part(slot, t), lat_recv.at[slot, t]).wait()

    def sp_copy(target):
        return pltpu.make_async_remote_copy(
            src_ref=latbuf.at[me, mine],
            dst_ref=latbuf.at[me, mine],
            send_sem=sp_send.at[target],
            recv_sem=lat_recv.at[me, mine],
            device_id={"sp": target},
            device_id_type=MESH,
        )

    def sp_start(target, carry):
        sp_copy(target).start()
        return carry

    lax.fori_loop(me + 1, sp, sp_start, 0)
    for k in range(1, tp):
        lat_copy(me, k).start()

    qlat[mine] = dot_nt(own, query_down[...]).astype(BF16)

    def q_copy(k):
        return pltpu.make_async_remote_copy(
            src_ref=qlat.at[mine],
            dst_ref=qlat.at[mine],
            send_sem=q_send.at[k],
            recv_sem=q_recv.at[mine],
            device_id={"tp": (mine + k) % tp},
            device_id_type=MESH,
        )

    for k in range(1, tp):
        q_copy(k).start()

    @pl.when(me == 0)
    def _():
        normed[pl.ds(0, HALO), :] = jnp.zeros((HALO, normed.shape[1]), BF16)

    @pl.when(me > 0)
    def _():
        halo_copy.wait_recv()
        normed[pl.ds(0, HALO), :] = normalized(halo[...], pre_gain[...]).astype(BF16)

    aligned = depth % 128 == 0

    def gate_step(i, slot, first=False):
        columns = pl.ds(pl.multiple_of(slot * depth, depth), depth)
        value = dot(normed[:, columns], wbuf[i, sp_row(slot), :])
        if first:
            acc[i] = value
        else:
            acc[i] += value

    if aligned:
        for i in range(3):
            gate_step(i, me, True)

    w_wait(late, pair)
    up(late, pair)
    down(late, pair)

    def forward(k):
        slot = me - k
        pltpu.make_async_copy(
            latbuf.at[slot, mine], latbuf.at[slot, mine], lat_recv.at[slot, mine]
        ).wait()
        for t in range(1, tp):
            lat_copy(slot, t).start()

    def forward_some(first, last):
        def one(k, carry):
            forward(k)
            return carry

        lax.fori_loop(first, jnp.minimum(last, me) + 1, one, 0)

    group = 2 * inner

    def line_step(d, carry):
        @pl.when(d > 1)
        def _():
            forward_some(group * (d - 2) + 1, group * (d - 1))

        for u in range(late + 1):

            @pl.when(zi - d >= 0)
            def _():
                slot = me - d * inner
                w_wait(u, slot)
                up(u, slot)
                if u < late:
                    w_copy(u, slot, 2).start()
                else:
                    w_wait(u, pair - d * inner)
                    up(u, pair - d * inner)

            @pl.when(zi + d <= lines - 1)
            def _():
                slot = me + d * inner
                w_wait(u, slot)
                down(u, slot)
                if u < late:
                    w_copy(u, slot, 2).start()
                else:
                    w_wait(u, pair + d * inner)
                    down(u, pair + d * inner)

        if aligned:

            @pl.when(zi - d >= 0)
            def _():
                for i in range(3):
                    gate_step(i, me - d * inner)

            @pl.when(zi + d <= lines - 1)
            def _():
                for i in range(3):
                    gate_step(i, me + d * inner)

        return carry

    lax.fori_loop(1, lines, line_step, 0)

    forward_some(group * (lines - 2) + 1, sp - 1)

    lane = lax.broadcasted_iota(jnp.int32, (rows, heads * NOPE), 1)
    width = heads * ROPE
    for k in range(1, tp):
        t = (mine + k) % tp
        pltpu.make_async_copy(qlat.at[t], qlat.at[t], q_recv.at[t]).wait()
    query_latent = jnp.concatenate([qlat[t].astype(F32) for t in range(tp)], axis=1)
    query_normed = normalized(query_latent, query_gain[...]).astype(BF16)
    query_nope = dot(query_normed, query_up[...])
    turned = dot_nt(query_normed, query_rotary[...])
    locals_[3].wait()
    turned = (turned * tab[:, :width] + swapped(turned) * tab[:, width : 2 * width]).astype(BF16)
    for h in range(heads):
        qnope[h] = jnp.where(lane // NOPE == h, query_nope, 0.0).astype(BF16)
        qturn[h] = turned[:, h * ROPE : (h + 1) * ROPE]

    factor = (NOPE + ROPE) ** (-0.5)

    def keys_of(slot):
        lat_wait(slot)
        latent = jnp.concatenate([latbuf[slot, t, 0:rows, 0:kl] for t in range(tp)], axis=1)
        latent_normed = normalized(latent, latent_gain[...]).astype(BF16)
        key_nope = dot(latent_normed, key_up[...]).astype(BF16)
        values = dot(latent_normed, value_up[...]).astype(BF16)
        return key_nope, values, latbuf[slot, mine, rows : rows + ROPE, 0:rows]

    def scores_of(h, key_nope, turned_keys):
        return (dot_nt(qnope[h], key_nope) + dot(qturn[h], turned_keys)) * factor

    key_nope, values, turned_keys = keys_of(me)
    row_id = lax.broadcasted_iota(jnp.int32, (rows, rows), 0)
    key_id = lax.broadcasted_iota(jnp.int32, (rows, rows), 1)
    for h in range(heads):
        scores = jnp.where(key_id <= row_id, scores_of(h, key_nope, turned_keys), -1e30)
        top = jnp.max(scores, axis=-1, keepdims=True)
        weights = jnp.where(key_id <= row_id, jnp.exp(scores - top), 0.0)
        best[h] = top
        total[h] = jnp.sum(weights, axis=-1, keepdims=True)
        weighted[h] = dot(weights.astype(BF16), values)

    def attend(k, carry):
        key_nope, values, turned_keys = keys_of(me - k)
        for h in range(heads):
            scores = scores_of(h, key_nope, turned_keys)
            old = best[h]
            top = jnp.maximum(old, jnp.max(scores, axis=-1, keepdims=True))
            weights = jnp.exp(scores - top)
            shrink = jnp.exp(old - top)
            best[h] = top
            total[h] = total[h] * shrink + jnp.sum(weights, axis=-1, keepdims=True)
            weighted[h] = weighted[h] * shrink + dot(weights.astype(BF16), values)
        return carry

    lax.fori_loop(1, me + 1, attend, 0)
    value_lane = lax.broadcasted_iota(jnp.int32, (rows, heads * VDIM), 1)
    heads_mixed = jnp.zeros((rows, heads * VDIM), F32)
    for h in range(heads):
        logsum = best[h] + jnp.log(total[h])
        row_logsum[h : h + 1, :] = jnp.transpose(jnp.broadcast_to(logsum, (rows, rows)))[0:1, :]
        heads_mixed = jnp.where(value_lane // VDIM == h, weighted[h] / total[h], heads_mixed)
    locals_[5].wait()
    proj[...] = dot(heads_mixed.astype(BF16), wheads[...])

    def pair_slot(slot):
        for u in range(late):
            w_wait(u, slot)
        if aligned:
            for i in range(3):
                gate_step(i, slot)

    pair_slot(pair)

    def pair_step(d, carry):
        @pl.when(zi - d >= 0)
        def _():
            pair_slot(pair - d * inner)

        @pl.when(zi + d <= lines - 1)
        def _():
            pair_slot(pair + d * inner)

        return carry

    lax.fori_loop(1, lines, pair_step, 0)
    if not aligned:
        for i in range(3):
            acc[i] = dot(normed[...], wbuf[i])

    prod[...] = (acc[1] * acc[2]).astype(BF16).astype(F32)
    convolved = prod[pl.ds(HALO - TAPS + 1, rows), :] * conv_taps[0:1, :]
    for k in range(1, TAPS):
        convolved = convolved + prod[pl.ds(HALO - TAPS + 1 + k, rows), :] * conv_taps[k : k + 1, :]
    convm[...] = (acc[0, pl.ds(HALO, rows), :] * convolved).astype(BF16)

    locals_[6].wait()
    part = rows // tp

    def share(target):
        where = pl.ds(pl.multiple_of(target * part, part), part)
        return proj[where, :] + dot(convm[where, :], wout[...])

    def rs_copy(k):
        return pltpu.make_async_remote_copy(
            src_ref=outbuf.at[k],
            dst_ref=rsbuf.at[mine],
            send_sem=rs_send.at[k],
            recv_sem=rs_recv.at[mine],
            device_id={"tp": (mine + k) % tp},
            device_id_type=MESH,
        )

    order = sorted(range(1, tp), key=lambda k: abs(k - tp // 2))
    for k in order:
        outbuf[k] = share((mine + k) % tp).astype(BF16)
        rs_copy(k).start()
    result = share(mine)
    for k in range(1, tp):
        other = (mine + k) % tp
        pltpu.make_async_copy(rsbuf.at[other], rsbuf.at[other], rs_recv.at[other]).wait()
        result = result + rsbuf[other].astype(F32)
    mixed[...] = normalized(result, post_gain[...]).astype(BF16)

    for k in range(1, tp):
        rs_copy(k).wait_send()
        q_copy(k).wait_send()

    def lat_end(slot, carry):
        for k in range(1, tp):
            lat_copy(slot, k).wait_send()
        return carry

    lax.fori_loop(0, me + 1, lat_end, 0)

    @pl.when(me < sp - 1)
    def _():
        halo_copy.wait_send()

    def sp_end(target, carry):
        sp_copy(target).wait_send()
        return carry

    lax.fori_loop(me + 1, sp, sp_end, 0)

    def line_ends(u, z, slot):
        @pl.when((z <= zi) & (zi < lines - 1))
        def _():
            w_copy(u, slot, 0).wait_send()

        @pl.when((z >= zi) & (zi > 0))
        def _():
            w_copy(u, slot, 1).wait_send()

    def w_end(z, carry):
        slot = z * inner + xi
        for u in range(late):
            w_copy(u, slot, 2).wait_send()
            line_ends(u, z, slot)
        for x in range(inner):
            line_ends(late, z, z * inner + x)
        return carry

    lax.fori_loop(0, lines, w_end, 0)
    w_copy(late, me, 2).wait_send()


def w_units(channels):
    half = channels // 2
    return (0, 0, channels), (1, 0, channels), (2, 0, half), (2, half, half)


def rope_tables(blocks, rows, heads):
    half = ROPE // 2
    frequency = np.float32(rope_theta) ** (-np.arange(half, dtype=np.float32) / np.float32(half))
    positions = np.arange(blocks * rows, dtype=np.float32)
    angles = positions[:, None] * frequency.astype(np.float32)
    cosine = np.concatenate([np.cos(angles)] * 2, 1)
    sine = np.concatenate([-np.sin(angles), np.sin(angles)], 1)
    table = np.concatenate([cosine] * heads + [sine] * heads, 1).astype(np.float32)
    keys = np.concatenate([cosine, sine], 1).astype(np.float32).reshape(blocks, rows, 2 * ROPE)
    return table.reshape(blocks, rows, -1), keys.transpose(0, 2, 1).copy()


def solution(mesh):
    sp, tp = mesh.shape["sp"], mesh.shape["tp"]
    inner = 2

    def local(
        tokens, pre_gain, outer_gate, inner_gate, conv_input, conv_taps, query_down, latent_down,
        rotary_down, query_gain, latent_gain, query_up, query_rotary, key_up, value_up,
        conv_output, heads_output, post_gain,
    ):
        rows, model = tokens.shape
        depth, channels = outer_gate.shape
        heads = query_up.shape[1] // NOPE
        ql, kl = query_down.shape[1], latent_down.shape[1]
        units = len(w_units(channels))
        part = rows // tp
        table, key_table = map(jnp.asarray, rope_tables(sp, rows, heads))
        vm = pl.BlockSpec(memory_space=pltpu.VMEM)
        hbm = pl.BlockSpec(memory_space=pl.ANY)
        dma = pltpu.SemaphoreType.DMA
        return pl.pallas_call(
            functools.partial(kernel, sp, tp, inner),
            out_shape=(
                jax.ShapeDtypeStruct((part, model), BF16),
                jax.ShapeDtypeStruct((heads, rows), F32),
            ),
            in_specs=[
                vm, vm, hbm, hbm, hbm, vm, vm, vm, vm, vm, vm, vm, vm, vm, vm, hbm, hbm, vm, hbm, hbm,
            ],
            out_specs=(vm, vm),
            scratch_shapes=[
                pltpu.VMEM((3, sp * depth, channels), BF16),
                pltpu.VMEM((rows + HALO, model), BF16),
                pltpu.VMEM((HALO, model), BF16),
                pltpu.VMEM((3, rows + HALO, channels), F32),
                pltpu.VMEM((rows + HALO, channels), F32),
                pltpu.VMEM((tp, rows, ql), BF16),
                pltpu.VMEM((sp, tp, rows + ROPE, max(kl, rows)), BF16),
                pltpu.VMEM((heads, rows, heads * NOPE), BF16),
                pltpu.VMEM((heads, rows, ROPE), BF16),
                pltpu.VMEM((heads, rows, 1), F32),
                pltpu.VMEM((heads, rows, 1), F32),
                pltpu.VMEM((heads, rows, heads * VDIM), F32),
                pltpu.VMEM((rows, model), F32),
                pltpu.VMEM((rows, channels), BF16),
                pltpu.VMEM((tp, part, model), BF16),
                pltpu.VMEM((tp, part, model), BF16),
                pltpu.VMEM(conv_output.shape, BF16),
                pltpu.VMEM(heads_output.shape, BF16),
                pltpu.VMEM((rows, 2 * heads * ROPE), F32),
                pltpu.VMEM((2 * ROPE, rows), F32),
                dma((7,)),
                dma((units, sp)),
                dma((3, units, sp)),
                dma((2,)),
                dma((tp,)),
                dma((tp,)),
                dma((sp, tp)),
                dma((sp, tp)),
                dma((sp,)),
                dma((tp,)),
                dma((tp,)),
            ],
            compiler_params=pltpu.CompilerParams(collective_id=0, has_side_effects=True),
        )(
            tokens, pre_gain.reshape(1, -1), outer_gate, inner_gate, conv_input, conv_taps,
            query_down.T, latent_down, rotary_down.T, query_gain.reshape(1, -1),
            latent_gain.reshape(1, -1), query_up, query_rotary.T, key_up, value_up,
            conv_output, heads_output, post_gain.reshape(1, -1), table, key_table,
        )

    in_specs = (
        P("sp", None), P(), P("sp", "tp"), P("sp", "tp"), P("sp", "tp"), P(None, "tp"),
        P(None, "tp"), P(None, "tp"), P(), P(), P(), P(None, "tp"), P(None, "tp"),
        P(None, "tp"), P(None, "tp"), P("tp", None), P("tp", None), P(),
    )
    out_specs = (P(("sp", "tp"), None), P("tp", "sp"))
    return jax.shard_map(local, mesh=mesh, in_specs=in_specs, out_specs=out_specs, check_vma=False)
```

```python
import functools

import jax
import jax.numpy as jnp
import numpy as np
from jax import lax
from jax.experimental import pallas as pl
from jax.experimental.pallas import tpu as pltpu
from jax.sharding import PartitionSpec as P

NOPE = 64
ROPE = 32
VDIM = 64
TAPS = 3
HALO = 16

eps = 1e-06
rope_theta = 500000.0
F32 = jnp.float32
BF16 = jnp.bfloat16
MESH = pl.DeviceIdType.MESH


def dot(a, b):
    return jnp.dot(a, b, preferred_element_type=F32)


def dot_nt(a, b):
    return lax.dot_general(a, b, (((1,), (1,)), ((), ())), preferred_element_type=F32)


def normalized(values, gain):
    wide = values.astype(F32)
    return wide * lax.rsqrt(jnp.mean(wide * wide, axis=-1, keepdims=True) + eps) * gain


def swapped(values):
    half = ROPE // 2
    parts = []
    for first in range(0, values.shape[-1], ROPE):
        parts += [values[:, first + half : first + ROPE], values[:, first : first + half]]
    return jnp.concatenate(parts, axis=1)


def kernel(
    sp, tp, inner,
    tokens, pre_gain, outer_gate, inner_gate, conv_input, conv_taps, query_down, latent_down,
    rotary_down, query_gain, latent_gain, query_up, query_rotary, key_up, value_up,
    conv_output, heads_output, post_gain, table, key_table,
    mixed, row_logsum,
    wbuf, normed, halo, acc, prod, qlat, latbuf, qnope, qturn, best, total, weighted, proj,
    convm, outbuf, rsbuf, wout, wheads, tab, key_tab,
    local_sem, w_recv, w_send, halo_sem, q_send, q_recv, lat_send, lat_recv, sp_send,
    rs_send, rs_recv,
):
    rows = tokens.shape[0]
    depth = outer_gate.shape[0]
    heads = query_up.shape[1] // NOPE
    lines = sp // inner
    me = lax.axis_index("sp")
    mine = lax.axis_index("tp")
    zi = me // inner
    xi = me % inner
    ql = query_down.shape[0]
    channels = outer_gate.shape[1]
    units = w_units(channels)
    kl = latent_down.shape[1]

    def sp_row(slot):
        return pl.ds(pl.multiple_of(slot * depth, depth), depth)

    locals_ = [
        pltpu.make_async_copy(ref, wbuf.at[i, sp_row(me)], local_sem.at[i])
        for i, ref in enumerate((outer_gate, inner_gate, conv_input))
    ]
    locals_ += [
        pltpu.make_async_copy(table.at[me], tab, local_sem.at[3]),
        pltpu.make_async_copy(key_table.at[me], key_tab, local_sem.at[6]),
        pltpu.make_async_copy(heads_output, wheads, local_sem.at[4]),
        pltpu.make_async_copy(conv_output, wout, local_sem.at[5]),
    ]
    for copy in locals_:
        copy.start()

    barrier = pltpu.get_barrier_semaphore()

    def greet_sp(k, carry):
        pl.semaphore_signal(barrier, inc=1, device_id={"sp": (me + k) % sp}, device_id_type=MESH)
        return carry

    lax.fori_loop(1, sp, greet_sp, 0)
    for k in range(1, tp):
        pl.semaphore_signal(barrier, inc=1, device_id={"tp": (mine + k) % tp}, device_id_type=MESH)

    normed[pl.ds(HALO, rows), :] = normalized(tokens[...], pre_gain[...]).astype(BF16)
    pl.semaphore_wait(barrier, sp + tp - 2)

    def w_part(u, slot):
        i, first, size = units[u]
        return wbuf.at[i, sp_row(slot), pl.ds(first, size)]

    def w_copy(u, slot, way):
        if way == 2:
            target = zi * inner + (inner - 1 - xi)
        else:
            target = me + (inner if way == 0 else -inner)
        return pltpu.make_async_remote_copy(
            src_ref=w_part(u, slot),
            dst_ref=w_part(u, slot),
            send_sem=w_send.at[way, u, slot],
            recv_sem=w_recv.at[u, slot],
            device_id={"sp": target},
            device_id_type=MESH,
        )

    def w_wait(u, slot):
        pltpu.make_async_copy(w_part(u, slot), w_part(u, slot), w_recv.at[u, slot]).wait()

    def up(u, slot):
        @pl.when(zi < lines - 1)
        def _():
            w_copy(u, slot, 0).start()

    def down(u, slot):
        @pl.when(zi > 0)
        def _():
            w_copy(u, slot, 1).start()

    late = len(units) - 1
    pair = zi * inner + (inner - 1 - xi)

    halo_copy = pltpu.make_async_remote_copy(
        src_ref=tokens.at[pl.ds(rows - HALO, HALO)],
        dst_ref=halo,
        send_sem=halo_sem.at[0],
        recv_sem=halo_sem.at[1],
        device_id={"sp": (me + 1) % sp},
        device_id_type=MESH,
    )

    @pl.when(me < sp - 1)
    def _():
        halo_copy.start()

    for i in range(3):
        locals_[i].wait()
    w_copy(late, me, 2).start()
    for u in range(late):
        up(u, me)
        down(u, me)
        w_copy(u, me, 2).start()
    up(late, me)
    down(late, me)

    own = normed[pl.ds(HALO, rows), :]
    latbuf[me, mine, 0:rows, 0:kl] = dot(own, latent_down[...]).astype(BF16)
    key_raw = dot_nt(rotary_down[...], own)
    half = ROPE // 2
    locals_[4].wait()
    key_swap = jnp.concatenate([key_raw[half:], key_raw[:half]], axis=0)
    key_rotary = key_raw * key_tab[0:ROPE, :] + key_swap * key_tab[ROPE : 2 * ROPE, :]
    latbuf[me, mine, rows : rows + ROPE, 0:rows] = key_rotary.astype(BF16)

    def lat_part(slot, t):
        return latbuf.at[slot, t, pl.ds(0, rows)]

    def lat_copy(slot, k):
        return pltpu.make_async_remote_copy(
            src_ref=lat_part(slot, mine),
            dst_ref=lat_part(slot, mine),
            send_sem=lat_send.at[slot, k],
            recv_sem=lat_recv.at[slot, mine],
            device_id={"tp": (mine + k) % tp},
            device_id_type=MESH,
        )

    def lat_wait(slot):
        for k in range(1, tp):
            t = (mine + k) % tp
            pltpu.make_async_copy(lat_part(slot, t), lat_part(slot, t), lat_recv.at[slot, t]).wait()

    def sp_copy(target):
        return pltpu.make_async_remote_copy(
            src_ref=latbuf.at[me, mine],
            dst_ref=latbuf.at[me, mine],
            send_sem=sp_send.at[target],
            recv_sem=lat_recv.at[me, mine],
            device_id={"sp": target},
            device_id_type=MESH,
        )

    def sp_start(target, carry):
        sp_copy(target).start()
        return carry

    lax.fori_loop(me + 1, sp, sp_start, 0)
    for k in range(1, tp):
        lat_copy(me, k).start()

    qlat[mine] = dot_nt(own, query_down[...]).astype(BF16)

    def q_copy(k):
        return pltpu.make_async_remote_copy(
            src_ref=qlat.at[mine],
            dst_ref=qlat.at[mine],
            send_sem=q_send.at[k],
            recv_sem=q_recv.at[mine],
            device_id={"tp": (mine + k) % tp},
            device_id_type=MESH,
        )

    for k in range(1, tp):
        q_copy(k).start()

    @pl.when(me == 0)
    def _():
        normed[pl.ds(0, HALO), :] = jnp.zeros((HALO, normed.shape[1]), BF16)

    @pl.when(me > 0)
    def _():
        halo_copy.wait_recv()
        normed[pl.ds(0, HALO), :] = normalized(halo[...], pre_gain[...]).astype(BF16)

    aligned = depth % 128 == 0

    def gate_step(i, slot, first=False):
        columns = pl.ds(pl.multiple_of(slot * depth, depth), depth)
        value = dot(normed[:, columns], wbuf[i, sp_row(slot), :])
        if first:
            acc[i] = value
        else:
            acc[i] += value

    if aligned:
        for i in range(3):
            gate_step(i, me, True)

    w_wait(late, pair)
    up(late, pair)
    down(late, pair)

    def forward(k):
        slot = me - k
        pltpu.make_async_copy(
            latbuf.at[slot, mine], latbuf.at[slot, mine], lat_recv.at[slot, mine]
        ).wait()
        for t in range(1, tp):
            lat_copy(slot, t).start()

    def forward_some(first, last):
        def one(k, carry):
            forward(k)
            return carry

        lax.fori_loop(first, jnp.minimum(last, me) + 1, one, 0)

    group = 2 * inner

    lane = lax.broadcasted_iota(jnp.int32, (rows, heads * NOPE), 1)
    width = heads * ROPE
    for k in range(1, tp):
        t = (mine + k) % tp
        pltpu.make_async_copy(qlat.at[t], qlat.at[t], q_recv.at[t]).wait()
    query_latent = jnp.concatenate([qlat[t].astype(F32) for t in range(tp)], axis=1)
    query_normed = normalized(query_latent, query_gain[...]).astype(BF16)
    query_nope = dot(query_normed, query_up[...])
    turned = dot_nt(query_normed, query_rotary[...])
    locals_[3].wait()
    turned = (turned * tab[:, :width] + swapped(turned) * tab[:, width : 2 * width]).astype(BF16)
    for h in range(heads):
        qnope[h] = jnp.where(lane // NOPE == h, query_nope, 0.0).astype(BF16)
        qturn[h] = turned[:, h * ROPE : (h + 1) * ROPE]

    factor = (NOPE + ROPE) ** (-0.5)

    def keys_of(slot):
        lat_wait(slot)
        latent = jnp.concatenate([latbuf[slot, t, 0:rows, 0:kl] for t in range(tp)], axis=1)
        latent_normed = normalized(latent, latent_gain[...]).astype(BF16)
        key_nope = dot(latent_normed, key_up[...]).astype(BF16)
        values = dot(latent_normed, value_up[...]).astype(BF16)
        return key_nope, values, latbuf[slot, mine, rows : rows + ROPE, 0:rows]

    def scores_of(h, key_nope, turned_keys):
        return (dot_nt(qnope[h], key_nope) + dot(qturn[h], turned_keys)) * factor

    key_nope, values, turned_keys = keys_of(me)
    row_id = lax.broadcasted_iota(jnp.int32, (rows, rows), 0)
    key_id = lax.broadcasted_iota(jnp.int32, (rows, rows), 1)
    for h in range(heads):
        scores = jnp.where(key_id <= row_id, scores_of(h, key_nope, turned_keys), -1e30)
        top = jnp.max(scores, axis=-1, keepdims=True)
        weights = jnp.where(key_id <= row_id, jnp.exp(scores - top), 0.0)
        best[h] = top
        total[h] = jnp.sum(weights, axis=-1, keepdims=True)
        weighted[h] = dot(weights.astype(BF16), values)

    def attend(k, carry):
        key_nope, values, turned_keys = keys_of(me - k)
        for h in range(heads):
            scores = scores_of(h, key_nope, turned_keys)
            old = best[h]
            top = jnp.maximum(old, jnp.max(scores, axis=-1, keepdims=True))
            weights = jnp.exp(scores - top)
            shrink = jnp.exp(old - top)
            best[h] = top
            total[h] = total[h] * shrink + jnp.sum(weights, axis=-1, keepdims=True)
            weighted[h] = weighted[h] * shrink + dot(weights.astype(BF16), values)
        return carry

    def pair_slot(slot):
        for u in range(late):
            w_wait(u, slot)
        if aligned:
            for i in range(3):
                gate_step(i, slot)

    def attend_some(first, last):
        lax.fori_loop(first, jnp.minimum(last, me) + 1, attend, 0)

    def pair_at(d):
        @pl.when(d == 0)
        def _():
            pair_slot(pair)

        @pl.when((d > 0) & (zi - d >= 0))
        def _():
            pair_slot(pair - d * inner)

        @pl.when((d > 0) & (zi + d <= lines - 1))
        def _():
            pair_slot(pair + d * inner)

    def line_step(d, carry):
        @pl.when(d > 1)
        def _():
            forward_some(group * (d - 2) + 1, group * (d - 1))

        for u in range(late + 1):
            if u == 2:

                @pl.when(d > 1)
                def _():
                    attend_some(group * (d - 2) + 1, group * (d - 1))
                    pair_at(d - 2)

            @pl.when(zi - d >= 0)
            def _():
                slot = me - d * inner
                w_wait(u, slot)
                up(u, slot)
                if u < late:
                    w_copy(u, slot, 2).start()
                else:
                    w_wait(u, pair - d * inner)
                    up(u, pair - d * inner)

            @pl.when(zi + d <= lines - 1)
            def _():
                slot = me + d * inner
                w_wait(u, slot)
                down(u, slot)
                if u < late:
                    w_copy(u, slot, 2).start()
                else:
                    w_wait(u, pair + d * inner)
                    down(u, pair + d * inner)

        if aligned:

            @pl.when(zi - d >= 0)
            def _():
                for i in range(3):
                    gate_step(i, me - d * inner)

            @pl.when(zi + d <= lines - 1)
            def _():
                for i in range(3):
                    gate_step(i, me + d * inner)

        return carry

    lax.fori_loop(1, lines, line_step, 0)

    forward_some(group * (lines - 2) + 1, sp - 1)

    attend_some(group * (lines - 2) + 1, sp - 1)
    value_lane = lax.broadcasted_iota(jnp.int32, (rows, heads * VDIM), 1)
    heads_mixed = jnp.zeros((rows, heads * VDIM), F32)
    for h in range(heads):
        logsum = best[h] + jnp.log(total[h])
        row_logsum[h : h + 1, :] = jnp.transpose(jnp.broadcast_to(logsum, (rows, rows)))[0:1, :]
        heads_mixed = jnp.where(value_lane // VDIM == h, weighted[h] / total[h], heads_mixed)
    locals_[5].wait()
    proj[...] = dot(heads_mixed.astype(BF16), wheads[...])

    def pair_end(d, carry):
        pair_at(d)
        return carry

    lax.fori_loop(max(0, lines - 2), lines, pair_end, 0)
    if not aligned:
        for i in range(3):
            acc[i] = dot(normed[...], wbuf[i])

    prod[...] = (acc[1] * acc[2]).astype(BF16).astype(F32)
    convolved = prod[pl.ds(HALO - TAPS + 1, rows), :] * conv_taps[0:1, :]
    for k in range(1, TAPS):
        convolved = convolved + prod[pl.ds(HALO - TAPS + 1 + k, rows), :] * conv_taps[k : k + 1, :]
    convm[...] = (acc[0, pl.ds(HALO, rows), :] * convolved).astype(BF16)

    locals_[6].wait()
    part = rows // tp

    def share(target):
        where = pl.ds(pl.multiple_of(target * part, part), part)
        return proj[where, :] + dot(convm[where, :], wout[...])

    def rs_copy(k):
        return pltpu.make_async_remote_copy(
            src_ref=outbuf.at[k],
            dst_ref=rsbuf.at[mine],
            send_sem=rs_send.at[k],
            recv_sem=rs_recv.at[mine],
            device_id={"tp": (mine + k) % tp},
            device_id_type=MESH,
        )

    order = sorted(range(1, tp), key=lambda k: abs(k - tp // 2))
    for k in order:
        outbuf[k] = share((mine + k) % tp).astype(BF16)
        rs_copy(k).start()
    result = share(mine)
    for k in range(1, tp):
        other = (mine + k) % tp
        pltpu.make_async_copy(rsbuf.at[other], rsbuf.at[other], rs_recv.at[other]).wait()
        result = result + rsbuf[other].astype(F32)
    mixed[...] = normalized(result, post_gain[...]).astype(BF16)

    for k in range(1, tp):
        rs_copy(k).wait_send()
        q_copy(k).wait_send()

    def lat_end(slot, carry):
        for k in range(1, tp):
            lat_copy(slot, k).wait_send()
        return carry

    lax.fori_loop(0, me + 1, lat_end, 0)

    @pl.when(me < sp - 1)
    def _():
        halo_copy.wait_send()

    def sp_end(target, carry):
        sp_copy(target).wait_send()
        return carry

    lax.fori_loop(me + 1, sp, sp_end, 0)

    def line_ends(u, z, slot):
        @pl.when((z <= zi) & (zi < lines - 1))
        def _():
            w_copy(u, slot, 0).wait_send()

        @pl.when((z >= zi) & (zi > 0))
        def _():
            w_copy(u, slot, 1).wait_send()

    def w_end(z, carry):
        slot = z * inner + xi
        for u in range(late):
            w_copy(u, slot, 2).wait_send()
            line_ends(u, z, slot)
        for x in range(inner):
            line_ends(late, z, z * inner + x)
        return carry

    lax.fori_loop(0, lines, w_end, 0)
    w_copy(late, me, 2).wait_send()


def w_units(channels):
    half = channels // 2
    return (0, 0, channels), (1, 0, channels), (2, 0, half), (2, half, half)


def rope_tables(blocks, rows, heads):
    half = ROPE // 2
    frequency = np.float32(rope_theta) ** (-np.arange(half, dtype=np.float32) / np.float32(half))
    positions = np.arange(blocks * rows, dtype=np.float32)
    angles = positions[:, None] * frequency.astype(np.float32)
    cosine = np.concatenate([np.cos(angles)] * 2, 1)
    sine = np.concatenate([-np.sin(angles), np.sin(angles)], 1)
    table = np.concatenate([cosine] * heads + [sine] * heads, 1).astype(np.float32)
    keys = np.concatenate([cosine, sine], 1).astype(np.float32).reshape(blocks, rows, 2 * ROPE)
    return table.reshape(blocks, rows, -1), keys.transpose(0, 2, 1).copy()


def solution(mesh):
    sp, tp = mesh.shape["sp"], mesh.shape["tp"]
    inner = 2

    def local(
        tokens, pre_gain, outer_gate, inner_gate, conv_input, conv_taps, query_down, latent_down,
        rotary_down, query_gain, latent_gain, query_up, query_rotary, key_up, value_up,
        conv_output, heads_output, post_gain,
    ):
        rows, model = tokens.shape
        depth, channels = outer_gate.shape
        heads = query_up.shape[1] // NOPE
        ql, kl = query_down.shape[1], latent_down.shape[1]
        units = len(w_units(channels))
        part = rows // tp
        table, key_table = map(jnp.asarray, rope_tables(sp, rows, heads))
        vm = pl.BlockSpec(memory_space=pltpu.VMEM)
        hbm = pl.BlockSpec(memory_space=pl.ANY)
        dma = pltpu.SemaphoreType.DMA
        return pl.pallas_call(
            functools.partial(kernel, sp, tp, inner),
            out_shape=(
                jax.ShapeDtypeStruct((part, model), BF16),
                jax.ShapeDtypeStruct((heads, rows), F32),
            ),
            in_specs=[
                vm, vm, hbm, hbm, hbm, vm, vm, vm, vm, vm, vm, vm, vm, vm, vm, hbm, hbm, vm, hbm, hbm,
            ],
            out_specs=(vm, vm),
            scratch_shapes=[
                pltpu.VMEM((3, sp * depth, channels), BF16),
                pltpu.VMEM((rows + HALO, model), BF16),
                pltpu.VMEM((HALO, model), BF16),
                pltpu.VMEM((3, rows + HALO, channels), F32),
                pltpu.VMEM((rows + HALO, channels), F32),
                pltpu.VMEM((tp, rows, ql), BF16),
                pltpu.VMEM((sp, tp, rows + ROPE, max(kl, rows)), BF16),
                pltpu.VMEM((heads, rows, heads * NOPE), BF16),
                pltpu.VMEM((heads, rows, ROPE), BF16),
                pltpu.VMEM((heads, rows, 1), F32),
                pltpu.VMEM((heads, rows, 1), F32),
                pltpu.VMEM((heads, rows, heads * VDIM), F32),
                pltpu.VMEM((rows, model), F32),
                pltpu.VMEM((rows, channels), BF16),
                pltpu.VMEM((tp, part, model), BF16),
                pltpu.VMEM((tp, part, model), BF16),
                pltpu.VMEM(conv_output.shape, BF16),
                pltpu.VMEM(heads_output.shape, BF16),
                pltpu.VMEM((rows, 2 * heads * ROPE), F32),
                pltpu.VMEM((2 * ROPE, rows), F32),
                dma((7,)),
                dma((units, sp)),
                dma((3, units, sp)),
                dma((2,)),
                dma((tp,)),
                dma((tp,)),
                dma((sp, tp)),
                dma((sp, tp)),
                dma((sp,)),
                dma((tp,)),
                dma((tp,)),
            ],
            compiler_params=pltpu.CompilerParams(collective_id=0, has_side_effects=True),
        )(
            tokens, pre_gain.reshape(1, -1), outer_gate, inner_gate, conv_input, conv_taps,
            query_down.T, latent_down, rotary_down.T, query_gain.reshape(1, -1),
            latent_gain.reshape(1, -1), query_up, query_rotary.T, key_up, value_up,
            conv_output, heads_output, post_gain.reshape(1, -1), table, key_table,
        )

    in_specs = (
        P("sp", None), P(), P("sp", "tp"), P("sp", "tp"), P("sp", "tp"), P(None, "tp"),
        P(None, "tp"), P(None, "tp"), P(), P(), P(), P(None, "tp"), P(None, "tp"),
        P(None, "tp"), P(None, "tp"), P("tp", None), P("tp", None), P(),
    )
    out_specs = (P(("sp", "tp"), None), P("tp", "sp"))
    return jax.shard_map(local, mesh=mesh, in_specs=in_specs, out_specs=out_specs, check_vma=False)
```
